32 devices in a mesh: ep: 16 (over z, y, x), tp: 2 (over core).
Axes of the slice: x: 2, y: 2, z: 4, core: 2. Of those that a mesh axis runs over, the one named last changes fastest.
Arguments:
- inputs: bfloat16 [256, 2048], P('ep'), may hold values from -6 to 6
- positions: int32 [256], P('ep'), may hold values from 1024 to 8191
- ret_state: float32 [256, 12, 128, 128], P('ep', 'tp'), may hold values from -4 to 4
- norm_mix: bfloat16 [2048], replicated, may hold values from 0.099609375 to 1.8984375
- w_query: bfloat16 [2048, 1536], P('ep', 'tp'), may hold values from -0.1875 to 0.1875
- w_key: bfloat16 [2048, 1536], P('ep', 'tp'), may hold values from -0.1875 to 0.1875
- w_value: bfloat16 [2048, 1536], P('ep', 'tp'), may hold values from -0.1875 to 0.1875
- w_gate_in: bfloat16 [2048, 1536], P('ep', 'tp'), may hold values from -0.1875 to 0.1875
- head_gain: bfloat16 [1536], P('tp'), may hold values from 0.099609375 to 1.8984375
- w_out: bfloat16 [1536, 2048], P('tp', 'ep'), may hold values from -0.15625 to 0.15625
- norm_ffn: bfloat16 [2048], replicated, may hold values from 0.099609375 to 1.8984375
- route_ids: int32 [256, 4], P('ep'), may hold values from 0 to 15, all different within a row; in each aligned block of 16 rows (0 to 15, 16 to 31, ...) at most 8 rows name the same one
- route_weight: bfloat16 [256, 4], P('ep'), may hold values from 0.19921875 to 1
- exp_gate: bfloat16 [16, 2048, 1024], P('ep', None, 'tp'), may hold values from -0.125 to 0.125
- exp_up: bfloat16 [16, 2048, 1024], P('ep', None, 'tp'), may hold values from -0.125 to 0.125
- exp_down: bfloat16 [16, 1024, 2048], P('ep', 'tp'), may hold values from -0.1875 to 0.1875
- dense_gate: bfloat16 [2048, 4096], P(None, ('ep', 'tp')), may hold values from -0.125 to 0.125
- dense_up: bfloat16 [2048, 4096], P(None, ('ep', 'tp')), may hold values from -0.125 to 0.125
- dense_down: bfloat16 [4096, 2048], P(('ep', 'tp')), may hold values from -0.1875 to 0.1875
- branch_gate: bfloat16 [2048], replicated, may hold values from -0.125 to 0.125
Outputs:
- layer_out: bfloat16 [256, 2048], P('ep')
- new_state: float32 [256, 12, 128, 128], P('ep', 'tp')
The draws below stay inside these ranges and needn't reach their ends.
Inputs may be any that keep to these rules, and one draw needn't show every extreme that they name: `route_ids`: each row names 4 different experts. Among the rows of one index of ep no expert is named more than 8 times, a bound that some block reaches.
All inputs are finite; a program needn't handle non-finite values.
Results may differ from the reference program's by a relative error of at most 0.015.
Values may be sent and summed in bfloat16 or wider, within the bound.
A program may use at most 128 MiB of HBM per device.

```python
import math
from functools import reduce
import jax
import jax.numpy as jnp
import numpy as np
from jax import lax

D = 2048
HEADS = 12
HEAD_DIM = 128
EXP_FF = 1024
DENSE_FF = 4096
TOP_K = 4
SEQ_DEV = 16
RET_WIDTH = 1536
EXPERTS = 16
TOKENS = 256
CAP = 8
N_EP = 16
N_TP = 2


def place_ends(drawn, stream_key, smallest, top_value):
    index_at = [jax.random.randint(jax.random.fold_in(stream_key, axis), (), 0, length) for axis, length in enumerate(drawn.shape)]
    longest = drawn.shape.index(max(drawn.shape))
    next_to = index_at[:longest] + [(index_at[longest] + 1) % drawn.shape[longest]] + index_at[longest + 1:]
    return drawn.at[tuple(index_at)].set(smallest).at[tuple(next_to)].set(top_value)


def raised(values, own_key, source, target, blocks, factor):
    def block_of(position):
        return (jnp.arange(values.shape[position]) // (values.shape[position] // blocks)).reshape((-1,) + (1,) * (values.ndim - 1 - position))

    first = jax.random.permutation(own_key, blocks)[block_of(target)]
    far = (block_of(target) + blocks // 2) % blocks
    return jnp.where((block_of(source) == first) | (block_of(source) == far), factor * values, values)


def block_scale(key, shape, shards, smallest, top_value):
    def one(axis_at, parts):
        draws = jax.random.uniform(jax.random.fold_in(jax.random.fold_in(key, 6), axis_at), (parts,), jnp.float32, smallest / len(shards), top_value / len(shards))
        return jnp.repeat(jnp.exp(draws), shape[axis_at] // parts).reshape((-1,) + (1,) * (len(shape) - axis_at - 1))

    loudness = one(*shards[0])
    for cut in shards[1:]:
        loudness = loudness * one(*cut)
    return loudness


def deal_out(rng, own, number, rows, amount, top, reach, lean):
    order = jax.random.permutation(rng, amount)
    heavy_load, ordinary = load_shares(amount, rows * top, reach, lean, True), load_shares(amount, rows * top, reach, lean, False)
    places = jnp.arange(amount)

    def named(lengths, turn):
        used = int((lengths > 0).sum())
        fixed = max(1, used // 4)
        moved = fixed + (places - fixed + turn * (used - fixed)) % max(1, amount - fixed)
        return jnp.zeros((amount,), jnp.int32).at[order[jnp.where(places < fixed, places, moved)]].set(jnp.asarray(lengths, jnp.int32))

    lengths = jnp.where(number % 4 == 0, named(heavy_load, number // 4), named(ordinary, number - number // 4 - 1))
    mixed = jax.random.permutation(jax.random.fold_in(own, 3), amount)
    giver, receiver = mixed[0:amount // 2 * 2:2], mixed[1:amount // 2 * 2:2]
    margin = jnp.minimum(lengths[giver] - 1, reach - lengths[receiver]) // 2
    margin = jnp.where((giver == order[0]) | (receiver == order[0]) | (lengths[receiver] == 0), 0, jnp.maximum(margin, 0))
    moved = jax.random.randint(jax.random.fold_in(own, 4), (amount // 2,), 0, 1 << 20) % (margin + 1)
    lengths = lengths.at[giver].add(-moved).at[receiver].add(moved)
    items = jnp.searchsorted(jnp.cumsum(lengths), jnp.arange(rows * top), side="right").astype(jnp.int32)
    grid = items.reshape(top, rows).T
    grid = grid[jax.random.permutation(jax.random.fold_in(own, 1), rows)]
    turn = jax.random.randint(jax.random.fold_in(own, 2), (rows, 1), 0, top)
    return jnp.take_along_axis(grid, (jnp.arange(top)[None, :] + turn) % top, axis=1)


def load_shares(amount, total, bound, slope, full):
    portions = [(1 << 20) // math.isqrt(standing ** slope) + 1 for standing in range(1, amount + 1)]
    largest = bound if full else min(bound, max(-(-total // amount), total * portions[0] // sum(portions)))
    least = 1 if total - largest >= amount - 1 else 0
    given, rest = [largest] + [least] * (amount - 1), total - largest - least * (amount - 1)
    while rest > 0:
        candidates = [i for i in range(1, amount) if given[i] < largest] or [i for i in range(1, amount) if given[i] < bound]
        pool, budget = sum([portions[i] for i in candidates]), rest
        for i in candidates:
            addition = min(bound - given[i], max(1, budget * portions[i] // pool), rest)
            given[i] = given[i] + addition
            rest = rest - addition
    return np.array(given)


def scatter_about(stream_key, dims, scale, bound, pieces=(), kind=jnp.bfloat16):
    drawn = jax.random.normal(stream_key, dims, jnp.float32) * scale
    if len(pieces) > 0:
        drawn = block_scale(stream_key, dims, pieces, -0.22, 0.18) * drawn
    return jnp.clip(drawn, min=-bound, max=bound).astype(kind)


def gaussian_with(key, dims, deviation, reach, shards, heavy, kind=jnp.bfloat16):
    values = deviation * jax.random.normal(key, dims, jnp.float32)
    if shards:
        values = values * block_scale(key, dims, shards, -0.22, 0.18)
    return jnp.clip(raised(values, jax.random.fold_in(key, 3), *heavy), -reach, reach).astype(kind)


def setup_inputs(seed: int = 0) -> dict:
    keys = jax.random.split(jax.random.key(seed), 21)
    inputs = scatter_about(keys[0], (TOKENS, D), 1.0, 6.0, ((0, 16),))
    positions = place_ends(jax.random.randint(keys[1], (TOKENS,), 1024, 8192), jax.random.fold_in(keys[1], 1), 1024, 8191).astype(jnp.int32)
    ret_state = scatter_about(keys[2], (TOKENS, HEADS, HEAD_DIM, HEAD_DIM), 0.25, 4.0, ((0, 16), (1, 2)), jnp.float32)
    norm_mix = jnp.clip(1.0 + 0.18 * jax.random.normal(keys[3], (D,), jnp.float32), 0.099609375, 1.8984375).astype(jnp.bfloat16)
    w_query = gaussian_with(keys[4], (D, RET_WIDTH), D ** -0.5, 0.1875, ((0, 16), (1, 2)), (0, 1, 16, 2.0))
    w_key = gaussian_with(keys[5], (D, RET_WIDTH), D ** -0.5, 0.1875, ((0, 16), (1, 2)), (0, 1, 16, 2.0))
    w_value = gaussian_with(keys[6], (D, RET_WIDTH), D ** -0.5, 0.1875, ((0, 16), (1, 2)), (0, 1, 16, 2.0))
    w_gate_in = gaussian_with(keys[7], (D, RET_WIDTH), D ** -0.5, 0.1875, ((0, 16), (1, 2)), (0, 1, 16, 2.0))
    head_gain = jnp.clip(1.0 + 0.18 * jax.random.normal(keys[8], (RET_WIDTH,), jnp.float32), 0.099609375, 1.8984375).astype(jnp.bfloat16)
    w_out = scatter_about(keys[9], (RET_WIDTH, D), RET_WIDTH ** -0.5, 0.15625, ((0, 2), (1, 16)))
    norm_ffn = jnp.clip(1.0 + 0.18 * jax.random.normal(keys[10], (D,), jnp.float32), 0.099609375, 1.8984375).astype(jnp.bfloat16)
    route_ids_keys = jax.random.split(jax.random.fold_in(keys[11], 1), TOKENS // SEQ_DEV)
    route_ids_turns = jax.random.permutation(jax.random.fold_in(keys[11], 3), TOKENS // SEQ_DEV)
    route_ids = jax.vmap(lambda own, number: deal_out(jax.random.fold_in(keys[11], 2), own, number, SEQ_DEV, EXPERTS, TOP_K, CAP, 2))(route_ids_keys, route_ids_turns).reshape((TOKENS, TOP_K))
    route_weight = jnp.clip(jnp.exp(math.log(1.0) - 1.6133518 * jax.random.uniform(keys[12], (TOKENS, TOP_K), jnp.float32) ** block_scale(keys[12], (TOKENS, TOP_K), ((0, 16),), -0.2, 0.2)), 0.19921875, 1.0).astype(jnp.bfloat16)
    exp_gate = scatter_about(keys[13], (EXPERTS, D, EXP_FF), D ** -0.5, 0.125, ((0, 16), (2, 2)))
    exp_up = scatter_about(keys[14], (EXPERTS, D, EXP_FF), D ** -0.5, 0.125, ((0, 16), (2, 2)))
    exp_down = scatter_about(keys[15], (EXPERTS, EXP_FF, D), EXP_FF ** -0.5, 0.1875, ((0, 16), (1, 2)))
    dense_gate = scatter_about(keys[16], (D, DENSE_FF), D ** -0.5, 0.125, ((1, 32),))
    dense_up = scatter_about(keys[17], (D, DENSE_FF), D ** -0.5, 0.125, ((1, 32),))
    dense_down = gaussian_with(keys[18], (DENSE_FF, D), DENSE_FF ** -0.5, 0.1875, ((0, 32),), (0, 1, 32, 2.75))
    branch_gate = scatter_about(keys[19], (D,), D ** -0.5, 0.125)
    return {"inputs": inputs, "positions": positions, "ret_state": ret_state, "norm_mix": norm_mix, "w_query": w_query, "w_key": w_key, "w_value": w_value, "w_gate_in": w_gate_in, "head_gain": head_gain, "w_out": w_out, "norm_ffn": norm_ffn, "route_ids": route_ids, "route_weight": route_weight, "exp_gate": exp_gate, "exp_up": exp_up, "exp_down": exp_down, "dense_gate": dense_gate, "dense_up": dense_up, "dense_down": dense_down, "branch_gate": branch_gate}


EPS = 1e-06

def rms_scale(values, scales):
    widened = values.astype(jnp.float32)
    scaled = widened * lax.rsqrt(lax.optimization_barrier(jnp.mean(widened * widened, axis=-1, keepdims=True)) + EPS)
    return (scaled * scales.astype(jnp.float32)).astype(jnp.bfloat16)

def rotary_angles(positions, head_dim):
    halfway = head_dim // 2
    frequency = 10000.0 ** (-jnp.arange(halfway, dtype=jnp.float32) * 2.0 / head_dim)
    return positions.astype(jnp.float32)[:, None] * frequency[None, :]

def rotate_heads(values, angles):
    halfway = values.shape[-1] // 2
    cosine = jnp.cos(angles)[:, None, :]
    sine_of = jnp.sin(angles)[:, None, :]
    leading = values[..., :halfway]
    trailing = values[..., halfway:]
    return jnp.concatenate([leading * cosine - trailing * sine_of, trailing * cosine + leading * sine_of], axis=-1)

def log_decay(head_count):
    spread = jnp.arange(head_count, dtype=jnp.float32) * (5.0 / max(head_count - 1, 1))
    return jnp.log1p(-2.0 ** (-5.0 - spread))

def retain(queries, keys_in, values_in, gate_pre, old_state, positions, scales, log_gamma):
    row_count, head_count, head_dim = (old_state.shape[0], old_state.shape[1], old_state.shape[2])
    angles = rotary_angles(positions, head_dim)
    rot_query = rotate_heads(queries.astype(jnp.float32).reshape(row_count, head_count, head_dim), angles)
    rot_key = rotate_heads(keys_in.astype(jnp.float32).reshape(row_count, head_count, head_dim), angles) * head_dim ** (-0.5)
    value_heads = values_in.astype(jnp.float32).reshape(row_count, head_count, head_dim)
    new_state = jnp.exp(log_gamma)[None, :, None, None] * old_state + rot_key[:, :, :, None] * value_heads[:, :, None, :]
    readout = jnp.einsum('shd,shdv->shv', rot_query, new_state, precision=lax.Precision.HIGHEST)
    centred = readout - lax.optimization_barrier(jnp.mean(readout, axis=-1, keepdims=True))
    normed = centred * lax.rsqrt(lax.optimization_barrier(jnp.mean(centred * centred, axis=-1, keepdims=True)) + EPS)
    normed = normed * scales.astype(jnp.float32).reshape(head_count, head_dim)
    gated_out = normed.reshape(row_count, head_count * head_dim) * jax.nn.silu(gate_pre.astype(jnp.float32))
    return (gated_out.astype(jnp.bfloat16), new_state)

def expert_total(normed_ffn, route_ids, route_share, exp_gate, exp_up, exp_down):
    token_count = normed_ffn.shape[0]
    flat_ids = route_ids.reshape(-1)
    flat_share = route_share.reshape(-1)
    most_rows = N_EP * CAP

    def one_expert(running, expert):
        matches = flat_ids == expert
        where_hit = jnp.nonzero(matches, size=most_rows, fill_value=0)[0].astype(jnp.int32)
        in_use = jnp.arange(most_rows, dtype=jnp.int32) < jnp.sum(matches.astype(jnp.int32))
        token_of = (where_hit // TOP_K).astype(jnp.int32)
        chosen = normed_ffn[token_of]
        gate_part = jnp.dot(chosen, exp_gate[expert], preferred_element_type=jnp.float32)
        up_part = jnp.dot(chosen, exp_up[expert], preferred_element_type=jnp.float32)
        hidden = (jax.nn.silu(gate_part) * up_part).astype(jnp.bfloat16)
        result = jnp.dot(hidden, exp_down[expert], preferred_element_type=jnp.float32)
        picked = flat_share[where_hit]
        weight = jnp.where(in_use, picked, jnp.zeros_like(picked))
        return (running.at[token_of].add(result * weight[:, None]), None)
    running, _ = lax.scan(one_expert, jnp.zeros((token_count, D), jnp.float32), jnp.arange(EXPERTS, dtype=jnp.int32))
    return running

def reference(inputs, positions, ret_state, norm_mix, w_query, w_key, w_value, w_gate_in, head_gain, w_out, norm_ffn, route_ids, route_weight, exp_gate, exp_up, exp_down, dense_gate, dense_up, dense_down, branch_gate):
    normed = rms_scale(inputs, norm_mix)
    queries = jnp.dot(normed, w_query, preferred_element_type=jnp.float32).astype(jnp.bfloat16)
    keys_new = jnp.dot(normed, w_key, preferred_element_type=jnp.float32).astype(jnp.bfloat16)
    values_new = jnp.dot(normed, w_value, preferred_element_type=jnp.float32).astype(jnp.bfloat16)
    gate_pre = jnp.dot(normed, w_gate_in, preferred_element_type=jnp.float32).astype(jnp.bfloat16)
    retained, new_state = retain(queries, keys_new, values_new, gate_pre, ret_state, positions, head_gain, log_decay(HEADS))
    group_width = RET_WIDTH // N_TP
    halves = [lax.optimization_barrier(jnp.dot(retained[:, member * group_width:(member + 1) * group_width], w_out[member * group_width:(member + 1) * group_width], preferred_element_type=jnp.float32).astype(jnp.bfloat16)).astype(jnp.float32) for member in range(N_TP)]
    mixer_out = reduce(jnp.add, halves).astype(jnp.bfloat16)
    residual_sum = (inputs.astype(jnp.float32) + mixer_out.astype(jnp.float32)).astype(jnp.bfloat16)
    normed_ffn = rms_scale(residual_sum, norm_ffn)
    dense_hidden = (jax.nn.silu(jnp.dot(normed_ffn, dense_gate, preferred_element_type=jnp.float32)) * jnp.dot(normed_ffn, dense_up, preferred_element_type=jnp.float32)).astype(jnp.bfloat16)
    dense_result = jnp.dot(dense_hidden, dense_down, preferred_element_type=jnp.float32)
    branch_open = jax.nn.sigmoid(jnp.dot(normed_ffn, branch_gate[:, None], preferred_element_type=jnp.float32))
    widened = route_weight.astype(jnp.float32)
    route_share = widened / lax.optimization_barrier(jnp.sum(widened, axis=-1, keepdims=True))
    experts_out = expert_total(normed_ffn, route_ids, route_share, exp_gate, exp_up, exp_down)
    layer_out = (residual_sum.astype(jnp.float32) + experts_out + branch_open * dense_result).astype(jnp.bfloat16)
    return (layer_out, new_state)
```

```python
import functools

import jax
import jax.numpy as jnp
from jax import lax
from jax.experimental import pallas as pl
from jax.experimental.pallas import tpu as pltpu
from jax.sharding import PartitionSpec as P

HEADS = 12
EPS = 1e-06
MESH = pl.DeviceIdType.MESH
LANES = 128
F32 = jnp.float32
BF16 = jnp.bfloat16
VMEM_LIMIT = 60 * 1024 * 1024


def rotary_angles(positions, head_dim):
    halfway = head_dim // 2
    frequency = 10000.0 ** (-jnp.arange(halfway, dtype=jnp.float32) * 2.0 / head_dim)
    return positions.astype(jnp.float32)[:, None] * frequency[None, :]


def log_decay(head_count):
    spread = jnp.arange(head_count, dtype=jnp.float32) * (5.0 / max(head_count - 1, 1))
    return jnp.log1p(-(2.0 ** (-5.0 - spread)))


def normalize(values, gain):
    scaled = values * lax.rsqrt(jnp.mean(values * values, axis=-1, keepdims=True) + EPS)
    return (scaled * gain.astype(F32)).astype(BF16)


def greet(n, me, tp, partner=None):
    barrier = pltpu.get_barrier_semaphore()

    @pl.loop(1, n)
    def _(k):
        pl.semaphore_signal(
            barrier, inc=1, device_id=(lax.rem(me + k, n), tp), device_id_type=MESH
        )

    if partner is not None:
        pl.semaphore_signal(barrier, inc=1, device_id=(me, partner), device_id_type=MESH)
    pl.semaphore_wait(barrier, n - 1 + (partner is not None))


def to_peer(src, dst, send, recv, k, ep, tp):
    return pltpu.make_async_remote_copy(
        src_ref=src,
        dst_ref=dst,
        send_sem=send.at[k],
        recv_sem=recv.at[k],
        device_id=(ep, tp),
        device_id_type=MESH,
    )


def scatter_start(n, me, tp, src, dst, send, recv):
    @pl.loop(1, n)
    def _(k):
        peer = lax.rem(me + k, n)
        to_peer(src.at[peer], dst.at[me], send, recv, k, peer, tp).start()


def scatter_wait(n, me, tp, src, dst, send, recv):
    @pl.loop(1, n)
    def _(k):
        peer = lax.rem(me + k, n)
        came = lax.rem(me + n - k, n)
        copy = to_peer(src.at[peer], dst.at[came], send, recv, k, peer, tp)
        copy.wait_send()
        copy.wait_recv()


def project_kernel(
    n, x_ref, gain_ref, share_ref, wq, wk, wv, wg, out_ref, share_out,
    blocks, columns, parts, landed, shares, send, recv,
):
    me, tp = lax.axis_index("ep"), lax.axis_index("tp")
    seqs, width = x_ref.shape
    block = width // n
    normed = normalize(x_ref[...].astype(F32), gain_ref[...])
    for j in range(n):
        blocks[j] = normed[:, j * block : (j + 1) * block]
    greet(n, me, tp)
    sems = lambda i: (send.at[i], recv.at[i])
    scatter_start(n, me, tp, blocks, columns, *sems(0))
    scatter_start(n, me, tp, share_ref, shares, *sems(1))
    columns[me] = blocks[me]
    shares[me] = share_ref[me]
    scatter_wait(n, me, tp, blocks, columns, *sems(0))
    rows = columns[...].reshape(n * seqs, block)
    local = wq.shape[1]
    for i, w in enumerate((wq, wk, wv, wg)):
        part = jnp.dot(rows, w[...], preferred_element_type=F32).astype(BF16)
        parts[:, :, i * local : (i + 1) * local] = part.reshape(n, seqs, local)
    scatter_start(n, me, tp, parts, landed, *sems(2))
    landed[me] = parts[me]
    scatter_wait(n, me, tp, share_ref, shares, *sems(1))
    share_out[...] = shares[...]
    scatter_wait(n, me, tp, parts, landed, *sems(2))
    for i in range(4):
        cut = slice(i * local, (i + 1) * local)
        total = lax.fori_loop(
            0,
            n,
            lambda j, acc: acc + landed[j, :, cut].astype(F32),
            jnp.zeros((seqs, local), F32),
        )
        out_ref[:, cut] = total.astype(BF16)


def project(n, x, gain, share, weights):
    seqs, width = x.shape
    cols = sum(w.shape[1] for w in weights)
    vmem = pl.BlockSpec(memory_space=pltpu.VMEM)
    return pl.pallas_call(
        functools.partial(project_kernel, n),
        out_shape=(
            jax.ShapeDtypeStruct((seqs, cols), BF16),
            jax.ShapeDtypeStruct(share.shape, F32),
        ),
        in_specs=[vmem] * 7,
        out_specs=(vmem, vmem),
        scratch_shapes=[
            pltpu.VMEM((n, seqs, width // n), BF16),
            pltpu.VMEM((n, seqs, width // n), BF16),
            pltpu.VMEM((n, seqs, cols), BF16),
            pltpu.VMEM((n, seqs, cols), BF16),
            pltpu.VMEM(share.shape, F32),
            pltpu.SemaphoreType.DMA((3, n)),
            pltpu.SemaphoreType.DMA((3, n)),
        ],
        compiler_params=pltpu.CompilerParams(
            collective_id=0, has_side_effects=True, vmem_limit_bytes=VMEM_LIMIT
        ),
    )(x, gain, share, *weights)


def retain_kernel(
    gamma_ref, q_ref, k_ref, v_ref, g_ref, gain_ref, cos_ref, sin_ref, state_ref,
    new_ref, out_ref, readout,
):
    seqs, dim = q_ref.shape
    gamma = gamma_ref[pl.program_id(0)]
    cos, sin = cos_ref[...], sin_ref[...]

    def rotated(ref):
        val = ref[...].astype(F32)
        return val * cos + pltpu.roll(val, dim // 2, 1) * sin

    query = rotated(q_ref).T
    key = (rotated(k_ref) * dim ** (-0.5)).T
    value = v_ref[...].astype(F32)
    for s in range(seqs):
        new = gamma * state_ref[s, 0] + key[:, s : s + 1] * value[s : s + 1, :]
        new_ref[s, 0] = new
        readout[s : s + 1, :] = jnp.sum(new * query[:, s : s + 1], axis=0, keepdims=True)
    read = readout[...]
    centred = read - jnp.mean(read, axis=-1, keepdims=True)
    normed = centred * lax.rsqrt(jnp.mean(centred * centred, axis=-1, keepdims=True) + EPS)
    gate = g_ref[...].astype(F32)
    out_ref[...] = (
        normed * gain_ref[...].astype(F32) * (gate * jax.nn.sigmoid(gate))
    ).astype(BF16)


def retain(gamma, joined, gain, cos, sin, state):
    seqs, heads, dim = state.shape[:3]
    piece = lambda i: pl.BlockSpec((seqs, dim), lambda h, i=i: (0, i * heads + h))
    whole = pl.BlockSpec((seqs, dim), lambda h: (0, 0))
    held = pl.BlockSpec((seqs, 1, dim, dim), lambda h: (0, h, 0, 0))
    return pl.pallas_call(
        retain_kernel,
        grid=(heads,),
        out_shape=(
            jax.ShapeDtypeStruct(state.shape, F32),
            jax.ShapeDtypeStruct((seqs, heads * dim), BF16),
        ),
        in_specs=[
            pl.BlockSpec(memory_space=pltpu.SMEM),
            piece(0), piece(1), piece(2), piece(3),
            pl.BlockSpec((1, dim), lambda h: (0, h)),
            whole, whole, held,
        ],
        out_specs=(held, pl.BlockSpec((seqs, dim), lambda h: (0, h))),
        scratch_shapes=[pltpu.VMEM((seqs, dim), F32)],
        compiler_params=pltpu.CompilerParams(vmem_limit_bytes=VMEM_LIMIT),
    )(gamma, joined, joined, joined, joined, gain, cos, sin, state)


def mix_kernel(
    n, x_ref, ret_ref, wout_ref, gain_ref, share_ref, open_w, eg_hbm, eu_hbm, ed_hbm,
    dg_hbm, du_hbm, dd_hbm, out_ref,
    heads, cols, cols_in, cols_sum, mixed, mixed_row, half_out, gathered, eg, eu, ed, dg, du, dd,
    hidden, dense_hidden, opening, other, other_in, own, summed, landed, final, final_in,
    load, send, recv, pair_send, pair_recv, relay_send, relay_recv,
):
    me, tp = lax.axis_index("ep"), lax.axis_index("tp")
    mate = 1 - tp
    seqs, width = x_ref.shape
    block, half = width // n, width // 2
    tokens = n * seqs
    loads = [
        pltpu.make_async_copy(src, dst, load.at[i])
        for i, (src, dst) in enumerate(
            ((eg_hbm.at[0], eg), (eu_hbm.at[0], eu), (dg_hbm, dg), (du_hbm, du),
             (ed_hbm.at[0], ed), (dd_hbm, dd))
        )
    ]
    for copy in loads:
        copy.start()
    greet(n, me, tp, mate)
    sems = lambda i: (send.at[i], recv.at[i])
    pair = lambda src, dst, i: to_peer(src, dst, pair_send, pair_recv, i, me, mate)

    @pl.loop(1, n)
    def _(k):
        peer = lax.rem(me + k, n)
        to_peer(ret_ref, heads.at[me], *sems(0), k, peer, tp).start()

    heads[me] = ret_ref[...]

    @pl.loop(1, n)
    def _(k):
        came = lax.rem(me + n - k, n)
        copy = to_peer(ret_ref, heads.at[came], *sems(0), k, lax.rem(me + k, n), tp)
        copy.wait_send()
        copy.wait_recv()

    part = jnp.dot(
        heads[...].reshape(tokens, ret_ref.shape[1]), wout_ref[...], preferred_element_type=F32
    )
    cols[...] = part.astype(BF16).reshape(n, seqs, block)
    swap = pair(cols, cols_in, 0)
    swap.start()
    swap.wait()
    cols_sum[...] = (cols[...].astype(F32) + cols_in[...].astype(F32)).astype(BF16)
    scatter_start(n, me, tp, cols_sum, mixed, *sems(1))
    mixed[me] = cols_sum[me]
    scatter_wait(n, me, tp, cols_sum, mixed, *sems(1))
    for j in range(n):
        mixed_row[:, j * block : (j + 1) * block] = mixed[j].astype(F32)
    residual = (x_ref[...].astype(F32) + mixed_row[...]).astype(BF16)
    mixed_row[...] = residual.astype(F32)
    normed = normalize(residual.astype(F32), gain_ref[...])
    for c in range(2):
        half_out[c] = normed[:, c * half : (c + 1) * half]

    @pl.loop(1, n)
    def _(k):
        peer = lax.rem(me + k, n)
        to_peer(half_out.at[tp], gathered.at[tp, me], *sems(2), k, peer, tp).start()

    for c in range(2):
        gathered[c, me] = half_out[c]

    @pl.loop(1, n)
    def _(k):
        came = lax.rem(me + n - k, n)
        copy = to_peer(
            half_out.at[tp], gathered.at[tp, came], *sems(2), k, lax.rem(me + k, n), tp
        )
        copy.wait_send()
        copy.wait_recv()
        to_peer(
            gathered.at[tp, came], gathered.at[tp, came], relay_send, relay_recv, k, me, mate
        ).start()

    for copy in loads:
        copy.wait()

    @pl.loop(1, n)
    def _(k):
        came = lax.rem(me + n - k, n)
        relay = to_peer(
            gathered.at[tp, came], gathered.at[mate, came], relay_send, relay_recv, k, me, mate
        )
        relay.wait_send()
        relay.wait_recv()

    def features(w, at):
        left = gathered[0].reshape(tokens, half)
        right = gathered[1].reshape(tokens, half)
        return jnp.dot(left, w[:half, at], preferred_element_type=F32) + jnp.dot(
            right, w[half:, at], preferred_element_type=F32
        )

    tile = min(256, eg.shape[1])

    @pl.loop(0, eg.shape[1] // tile)
    def _(j):
        at = pl.ds(pl.multiple_of(j * tile, tile), tile)
        gate = features(eg, at)
        hidden[:, at] = (gate * jax.nn.sigmoid(gate) * features(eu, at)).astype(BF16)

    every = slice(None)
    gate = features(dg, every)
    dense_hidden[...] = (gate * jax.nn.sigmoid(gate) * features(du, every)).astype(BF16)
    opening[...] = jax.nn.sigmoid(features(open_w, every))

    def branch(at):
        expert = jnp.dot(hidden[...], ed[:, at], preferred_element_type=F32)
        dense = jnp.dot(dense_hidden[...], dd[:, at], preferred_element_type=F32)
        share = share_ref[...].reshape(tokens, LANES)[:, :1]
        return expert * share + dense * opening[:, :1]

    wide = min(256, half)

    @pl.loop(0, half // wide)
    def _(j):
        src = pl.ds(pl.multiple_of(mate * half + j * wide, wide), wide)
        at = pl.ds(pl.multiple_of(j * wide, wide), wide)
        other[:, at] = branch(src).astype(BF16)

    swap = pair(other, other_in, 1)
    swap.start()

    @pl.loop(0, half // wide)
    def _(j):
        src = pl.ds(pl.multiple_of(tp * half + j * wide, wide), wide)
        at = pl.ds(pl.multiple_of(j * wide, wide), wide)
        own[:, at] = branch(src)

    swap.wait()
    summed[...] = (own[...] + other_in[...].astype(F32)).astype(BF16).reshape(n, seqs, half)
    scatter_start(n, me, tp, summed, landed, *sems(3))
    landed[me] = summed[me]
    scatter_wait(n, me, tp, summed, landed, *sems(3))
    total = lax.fori_loop(
        0, n, lambda j, acc: acc + landed[j].astype(F32), jnp.zeros((seqs, half), F32)
    )
    mine = mixed_row[:, pl.ds(pl.multiple_of(tp * half, half), half)]
    final[...] = (mine + total).astype(BF16)
    swap = pair(final, final_in, 2)
    swap.start()
    out_ref[:, pl.ds(pl.multiple_of(tp * half, half), half)] = final[...]
    swap.wait()
    out_ref[:, pl.ds(pl.multiple_of(mate * half, half), half)] = final_in[...]


def mix(n, x, retained, w_out, gain, share, open_w, weights):
    seqs, width = x.shape
    block, half, tokens = width // n, width // 2, n * seqs
    eg, eu, ed, dg, du, dd = weights
    vmem = pl.BlockSpec(memory_space=pltpu.VMEM)
    hbm = pl.BlockSpec(memory_space=pl.ANY)
    return pl.pallas_call(
        functools.partial(mix_kernel, n),
        out_shape=jax.ShapeDtypeStruct((seqs, width), BF16),
        in_specs=[vmem] * 6 + [hbm] * 6,
        out_specs=vmem,
        scratch_shapes=[
            pltpu.VMEM((n,) + retained.shape, BF16),
            pltpu.VMEM((n, seqs, block), BF16),
            pltpu.VMEM((n, seqs, block), BF16),
            pltpu.VMEM((n, seqs, block), BF16),
            pltpu.VMEM((n, seqs, block), BF16),
            pltpu.VMEM((seqs, width), F32),
            pltpu.VMEM((2, seqs, half), BF16),
            pltpu.VMEM((2, n, seqs, half), BF16),
            pltpu.VMEM(eg.shape[1:], BF16),
            pltpu.VMEM(eu.shape[1:], BF16),
            pltpu.VMEM(ed.shape[1:], BF16),
            pltpu.VMEM(dg.shape, BF16),
            pltpu.VMEM(du.shape, BF16),
            pltpu.VMEM(dd.shape, BF16),
            pltpu.VMEM((tokens, eg.shape[2]), BF16),
            pltpu.VMEM((tokens, dg.shape[1]), BF16),
            pltpu.VMEM((tokens, LANES), F32),
            pltpu.VMEM((tokens, half), BF16),
            pltpu.VMEM((tokens, half), BF16),
            pltpu.VMEM((tokens, half), F32),
            pltpu.VMEM((n, seqs, half), BF16),
            pltpu.VMEM((n, seqs, half), BF16),
            pltpu.VMEM((seqs, half), BF16),
            pltpu.VMEM((seqs, half), BF16),
            pltpu.SemaphoreType.DMA((6,)),
            pltpu.SemaphoreType.DMA((4, n)),
            pltpu.SemaphoreType.DMA((4, n)),
            pltpu.SemaphoreType.DMA((3,)),
            pltpu.SemaphoreType.DMA((3,)),
            pltpu.SemaphoreType.DMA((n,)),
            pltpu.SemaphoreType.DMA((n,)),
        ],
        compiler_params=pltpu.CompilerParams(
            collective_id=1, has_side_effects=True, vmem_limit_bytes=VMEM_LIMIT
        ),
    )(x, retained, w_out, gain, share, open_w, *weights)


def on_device(
    inputs,
    positions,
    ret_state,
    norm_mix,
    w_query,
    w_key,
    w_value,
    w_gate_in,
    head_gain,
    w_out,
    norm_ffn,
    route_ids,
    route_weight,
    exp_gate,
    exp_up,
    exp_down,
    dense_gate,
    dense_up,
    dense_down,
    branch_gate,
):
    n = lax.axis_size("ep")
    seqs, width = inputs.shape
    local_heads, head_dim = ret_state.shape[1], ret_state.shape[2]
    assert exp_gate.shape[0] == 1

    widened = route_weight.astype(F32)
    share = widened / jnp.sum(widened, axis=-1, keepdims=True)
    match = route_ids[None, :, :] == jnp.arange(n, dtype=jnp.int32)[:, None, None]
    by_expert = jnp.sum(jnp.where(match, share[None], 0.0), axis=2)
    by_expert = jnp.broadcast_to(by_expert[:, :, None], (n, seqs, LANES))
    angles = rotary_angles(positions, head_dim)
    cos, sin = jnp.cos(angles), jnp.sin(angles)
    cos = jnp.concatenate([cos, cos], axis=1)
    sin = jnp.concatenate([-sin, sin], axis=1)
    gamma = jnp.exp(
        lax.dynamic_slice_in_dim(
            log_decay(HEADS), lax.axis_index("tp") * local_heads, local_heads
        )
    )
    open_w = jnp.broadcast_to(branch_gate[:, None], (width, LANES))

    joined, shares = project(
        n, inputs, norm_mix[None, :], by_expert, (w_query, w_key, w_value, w_gate_in)
    )
    new_state, retained = retain(gamma, joined, head_gain[None, :], cos, sin, ret_state)
    layer_out = mix(
        n, inputs, retained, w_out, norm_ffn[None, :], shares, open_w,
        (exp_gate, exp_up, exp_down, dense_gate, dense_up, dense_down),
    )
    return (layer_out, new_state)


def solution(mesh):
    in_specs = (
        P("ep", None),
        P("ep"),
        P("ep", "tp", None, None),
        P(),
        P("ep", "tp"),
        P("ep", "tp"),
        P("ep", "tp"),
        P("ep", "tp"),
        P("tp"),
        P("tp", "ep"),
        P(),
        P("ep", None),
        P("ep", None),
        P("ep", None, "tp"),
        P("ep", None, "tp"),
        P("ep", "tp", None),
        P(None, ("ep", "tp")),
        P(None, ("ep", "tp")),
        P(("ep", "tp"), None),
        P(),
    )
    out_specs = (P("ep", None), P("ep", "tp", None, None))
    return jax.shard_map(
        on_device, mesh=mesh, in_specs=in_specs, out_specs=out_specs, check_vma=False
    )
```

```python
import functools

import jax
import jax.numpy as jnp
from jax import lax
from jax.experimental import pallas as pl
from jax.experimental.pallas import tpu as pltpu
from jax.sharding import PartitionSpec as P

HEADS = 12
EPS = 1e-06
MESH = pl.DeviceIdType.MESH
LANES = 128
F32 = jnp.float32
BF16 = jnp.bfloat16
VMEM_LIMIT = 60 * 1024 * 1024


def rotary_angles(positions, head_dim):
    halfway = head_dim // 2
    frequency = 10000.0 ** (-jnp.arange(halfway, dtype=jnp.float32) * 2.0 / head_dim)
    return positions.astype(jnp.float32)[:, None] * frequency[None, :]


def log_decay(head_count):
    spread = jnp.arange(head_count, dtype=jnp.float32) * (5.0 / max(head_count - 1, 1))
    return jnp.log1p(-(2.0 ** (-5.0 - spread)))


def normalize(values, gain):
    scaled = values * lax.rsqrt(jnp.mean(values * values, axis=-1, keepdims=True) + EPS)
    return (scaled * gain.astype(F32)).astype(BF16)


def greet(n, me, tp, partner=None):
    barrier = pltpu.get_barrier_semaphore()

    @pl.loop(1, n)
    def _(k):
        pl.semaphore_signal(
            barrier, inc=1, device_id=(lax.rem(me + k, n), tp), device_id_type=MESH
        )

    if partner is not None:
        pl.semaphore_signal(barrier, inc=1, device_id=(me, partner), device_id_type=MESH)
    pl.semaphore_wait(barrier, n - 1 + (partner is not None))


def to_peer(src, dst, send, recv, k, ep, tp):
    return pltpu.make_async_remote_copy(
        src_ref=src,
        dst_ref=dst,
        send_sem=send.at[k],
        recv_sem=recv.at[k],
        device_id=(ep, tp),
        device_id_type=MESH,
    )


def scatter_start(n, me, tp, src, dst, send, recv):
    @pl.loop(1, n)
    def _(k):
        peer = lax.rem(me + k, n)
        to_peer(src.at[peer], dst.at[me], send, recv, k, peer, tp).start()


def scatter_wait(n, me, tp, src, dst, send, recv):
    @pl.loop(1, n)
    def _(k):
        peer = lax.rem(me + k, n)
        came = lax.rem(me + n - k, n)
        copy = to_peer(src.at[peer], dst.at[came], send, recv, k, peer, tp)
        copy.wait_send()
        copy.wait_recv()


def project_kernel(
    n, x_ref, gain_ref, ids_ref, weight_ref, wq, wk, wv, wg, out_ref, share_out,
    blocks, columns, parts, plane, reduced, landed, share_ref, shares,
    send, recv, plane_send, plane_recv, line_send, line_recv,
):
    me, tp = lax.axis_index("ep"), lax.axis_index("tp")
    seqs, width = x_ref.shape
    block, local = width // n, wq.shape[1]
    outer, inner = parts.shape[2], parts.shape[1]
    along, inside = me // inner, lax.rem(me, inner)
    normed = normalize(x_ref[...].astype(F32), gain_ref[...])
    for j in range(n):
        blocks[j] = normed[:, j * block : (j + 1) * block]
    greet(n, me, tp)
    sems = lambda i: (send.at[i], recv.at[i])
    scatter_start(n, me, tp, blocks, columns, *sems(0))
    columns[me] = blocks[me]
    widened = weight_ref[...].astype(F32)
    part = widened / jnp.sum(widened, axis=-1, keepdims=True)
    for j in range(n):
        mine = jnp.sum(jnp.where(ids_ref[...] == j, part, 0.0), axis=-1, keepdims=True)
        share_ref[j] = jnp.broadcast_to(mine, (seqs, LANES))
    scatter_start(n, me, tp, share_ref, shares, *sems(1))
    shares[me] = share_ref[me]
    scatter_wait(n, me, tp, blocks, columns, *sems(0))
    rows = columns[...].reshape(n * seqs, block)

    def in_plane(i, k, source):
        peer = lax.rem(inside + k, inner)
        return to_peer(
            parts.at[i, peer], plane.at[i, source], plane_send.at[i], plane_recv.at[i], k,
            me - inside + peer, tp,
        )

    def in_line(i, k, source):
        peer = lax.rem(along + k, outer)
        return to_peer(
            reduced.at[i, peer], landed.at[i, source], line_send.at[i], line_recv.at[i], k,
            peer * inner + inside, tp,
        )

    span = inner * seqs
    for i, w in enumerate((wq, wk, wv, wg)):
        product = jnp.dot(rows, w[...], preferred_element_type=F32).astype(BF16)
        for z in range(outer):
            parts[i, :, z] = product[z * span : (z + 1) * span].reshape(inner, seqs, local)

        @pl.loop(1, inner)
        def _(k):
            in_plane(i, k, inside).start()

        plane[i, inside] = parts[i, inside]

    for i in range(4):

        @pl.loop(1, inner)
        def _(k):
            copy = in_plane(i, k, lax.rem(inside + inner - k, inner))
            copy.wait_send()
            copy.wait_recv()

        for z in range(outer):
            total = lax.fori_loop(
                0,
                inner,
                lambda j, acc: acc + plane[i, j, z].astype(F32),
                jnp.zeros((seqs, local), F32),
            )
            reduced[i, z] = total.astype(BF16)

        @pl.loop(1, outer)
        def _(k):
            in_line(i, k, along).start()

        landed[i, along] = reduced[i, along]

    scatter_wait(n, me, tp, share_ref, shares, *sems(1))
    share_out[...] = shares[...]
    for i in range(4):

        @pl.loop(1, outer)
        def _(k):
            copy = in_line(i, k, lax.rem(along + outer - k, outer))
            copy.wait_send()
            copy.wait_recv()

        total = lax.fori_loop(
            0,
            outer,
            lambda j, acc: acc + landed[i, j].astype(F32),
            jnp.zeros((seqs, local), F32),
        )
        out_ref[:, i * local : (i + 1) * local] = total.astype(BF16)


def project(n, x, gain, ids, weight, weights):
    seqs, width = x.shape
    local = weights[0].shape[1]
    outer = 4 if n % 4 == 0 else 1
    inner = n // outer
    vmem = pl.BlockSpec(memory_space=pltpu.VMEM)
    sem = pltpu.SemaphoreType.DMA
    return pl.pallas_call(
        functools.partial(project_kernel, n),
        out_shape=(
            jax.ShapeDtypeStruct((seqs, 4 * local), BF16),
            jax.ShapeDtypeStruct((n, seqs, LANES), F32),
        ),
        in_specs=[vmem] * 8,
        out_specs=(vmem, vmem),
        scratch_shapes=[
            pltpu.VMEM((n, seqs, width // n), BF16),
            pltpu.VMEM((n, seqs, width // n), BF16),
            pltpu.VMEM((4, inner, outer, seqs, local), BF16),
            pltpu.VMEM((4, inner, outer, seqs, local), BF16),
            pltpu.VMEM((4, outer, seqs, local), BF16),
            pltpu.VMEM((4, outer, seqs, local), BF16),
            pltpu.VMEM((n, seqs, LANES), F32),
            pltpu.VMEM((n, seqs, LANES), F32),
            sem((2, n)),
            sem((2, n)),
            sem((4, inner)),
            sem((4, inner)),
            sem((4, outer)),
            sem((4, outer)),
        ],
        compiler_params=pltpu.CompilerParams(
            collective_id=0, has_side_effects=True, vmem_limit_bytes=VMEM_LIMIT
        ),
    )(x, gain, ids, weight, *weights)


def retain_kernel(
    gamma_ref, q_ref, k_ref, v_ref, g_ref, gain_ref, cos_ref, sin_ref, state_ref,
    new_ref, out_ref, readout,
):
    seqs, dim = q_ref.shape
    gamma = gamma_ref[pl.program_id(0)]
    cos, sin = cos_ref[...], sin_ref[...]

    def rotated(ref):
        val = ref[...].astype(F32)
        return val * cos + pltpu.roll(val, dim // 2, 1) * sin

    query = rotated(q_ref).T
    key = (rotated(k_ref) * dim ** (-0.5)).T
    value = v_ref[...].astype(F32)
    for s in range(seqs):
        new = gamma * state_ref[s, 0] + key[:, s : s + 1] * value[s : s + 1, :]
        new_ref[s, 0] = new
        readout[s : s + 1, :] = jnp.sum(new * query[:, s : s + 1], axis=0, keepdims=True)
    read = readout[...]
    centred = read - jnp.mean(read, axis=-1, keepdims=True)
    normed = centred * lax.rsqrt(jnp.mean(centred * centred, axis=-1, keepdims=True) + EPS)
    gate = g_ref[...].astype(F32)
    out_ref[...] = (
        normed * gain_ref[...].astype(F32) * (gate * jax.nn.sigmoid(gate))
    ).astype(BF16)


def retain(gamma, joined, gain, cos, sin, state):
    seqs, heads, dim = state.shape[:3]
    piece = lambda i: pl.BlockSpec((seqs, dim), lambda h, i=i: (0, i * heads + h))
    whole = pl.BlockSpec((seqs, dim), lambda h: (0, 0))
    held = pl.BlockSpec((seqs, 1, dim, dim), lambda h: (0, h, 0, 0))
    return pl.pallas_call(
        retain_kernel,
        grid=(heads,),
        out_shape=(
            jax.ShapeDtypeStruct(state.shape, F32),
            jax.ShapeDtypeStruct((seqs, heads * dim), BF16),
        ),
        in_specs=[
            pl.BlockSpec(memory_space=pltpu.SMEM),
            piece(0), piece(1), piece(2), piece(3),
            pl.BlockSpec((1, dim), lambda h: (0, h)),
            whole, whole, held,
        ],
        out_specs=(held, pl.BlockSpec((seqs, dim), lambda h: (0, h))),
        scratch_shapes=[pltpu.VMEM((seqs, dim), F32)],
        compiler_params=pltpu.CompilerParams(vmem_limit_bytes=VMEM_LIMIT),
    )(gamma, joined, joined, joined, joined, gain, cos, sin, state)


def mix_kernel(
    n, x_ref, ret_ref, wout_ref, gain_ref, share_ref, open_w, eg_hbm, eu_hbm, ed_hbm,
    dg_hbm, du_hbm, dd_hbm, out_ref,
    heads, cols, cols_in, cols_sum, mixed, mixed_row, half_out, gathered, eg, eu, ed, dg, du, dd,
    hidden, dense_hidden, opening, other, other_in, own, summed, landed, final, final_in,
    load, send, recv, pair_send, pair_recv, relay_send, relay_recv,
):
    me, tp = lax.axis_index("ep"), lax.axis_index("tp")
    mate = 1 - tp
    seqs, width = x_ref.shape
    block, half = width // n, width // 2
    tokens = n * seqs
    loads = [
        pltpu.make_async_copy(src, dst, load.at[i])
        for i, (src, dst) in enumerate(
            ((eg_hbm.at[0], eg), (eu_hbm.at[0], eu), (dg_hbm, dg), (du_hbm, du),
             (ed_hbm.at[0], ed), (dd_hbm, dd))
        )
    ]
    for copy in loads:
        copy.start()
    greet(n, me, tp, mate)
    sems = lambda i: (send.at[i], recv.at[i])
    pair = lambda src, dst, i: to_peer(src, dst, pair_send, pair_recv, i, me, mate)

    @pl.loop(1, n)
    def _(k):
        peer = lax.rem(me + k, n)
        to_peer(ret_ref, heads.at[me], *sems(0), k, peer, tp).start()

    heads[me] = ret_ref[...]

    @pl.loop(1, n)
    def _(k):
        came = lax.rem(me + n - k, n)
        copy = to_peer(ret_ref, heads.at[came], *sems(0), k, lax.rem(me + k, n), tp)
        copy.wait_send()
        copy.wait_recv()

    part = jnp.dot(
        heads[...].reshape(tokens, ret_ref.shape[1]), wout_ref[...], preferred_element_type=F32
    )
    cols[...] = part.astype(BF16).reshape(n, seqs, block)
    swap = pair(cols, cols_in, 0)
    swap.start()
    swap.wait()
    cols_sum[...] = (cols[...].astype(F32) + cols_in[...].astype(F32)).astype(BF16)
    scatter_start(n, me, tp, cols_sum, mixed, *sems(1))
    mixed[me] = cols_sum[me]
    scatter_wait(n, me, tp, cols_sum, mixed, *sems(1))
    for j in range(n):
        mixed_row[:, j * block : (j + 1) * block] = mixed[j].astype(F32)
    residual = (x_ref[...].astype(F32) + mixed_row[...]).astype(BF16)
    mixed_row[...] = residual.astype(F32)
    normed = normalize(residual.astype(F32), gain_ref[...])
    for c in range(2):
        half_out[c] = normed[:, c * half : (c + 1) * half]

    @pl.loop(1, n)
    def _(k):
        peer = lax.rem(me + k, n)
        to_peer(half_out.at[tp], gathered.at[tp, me], *sems(2), k, peer, tp).start()

    for c in range(2):
        gathered[c, me] = half_out[c]

    @pl.loop(1, n)
    def _(k):
        came = lax.rem(me + n - k, n)
        copy = to_peer(
            half_out.at[tp], gathered.at[tp, came], *sems(2), k, lax.rem(me + k, n), tp
        )
        copy.wait_send()
        copy.wait_recv()
        to_peer(
            gathered.at[tp, came], gathered.at[tp, came], relay_send, relay_recv, k, me, mate
        ).start()

    for copy in loads:
        copy.wait()

    @pl.loop(1, n)
    def _(k):
        came = lax.rem(me + n - k, n)
        relay = to_peer(
            gathered.at[tp, came], gathered.at[mate, came], relay_send, relay_recv, k, me, mate
        )
        relay.wait_send()
        relay.wait_recv()

    def features(w, at):
        left = gathered[0].reshape(tokens, half)
        right = gathered[1].reshape(tokens, half)
        return jnp.dot(left, w[:half, at], preferred_element_type=F32) + jnp.dot(
            right, w[half:, at], preferred_element_type=F32
        )

    tile = min(256, eg.shape[1])

    @pl.loop(0, eg.shape[1] // tile)
    def _(j):
        at = pl.ds(pl.multiple_of(j * tile, tile), tile)
        gate = features(eg, at)
        hidden[:, at] = (gate * jax.nn.sigmoid(gate) * features(eu, at)).astype(BF16)

    every = slice(None)
    gate = features(dg, every)
    dense_hidden[...] = (gate * jax.nn.sigmoid(gate) * features(du, every)).astype(BF16)
    opening[...] = jax.nn.sigmoid(features(open_w, every))

    def branch(at):
        expert = jnp.dot(hidden[...], ed[:, at], preferred_element_type=F32)
        dense = jnp.dot(dense_hidden[...], dd[:, at], preferred_element_type=F32)
        share = share_ref[...].reshape(tokens, LANES)[:, :1]
        return expert * share + dense * opening[:, :1]

    wide = min(256, half)

    @pl.loop(0, half // wide)
    def _(j):
        src = pl.ds(pl.multiple_of(mate * half + j * wide, wide), wide)
        at = pl.ds(pl.multiple_of(j * wide, wide), wide)
        other[:, at] = branch(src).astype(BF16)

    swap = pair(other, other_in, 1)
    swap.start()

    @pl.loop(0, half // wide)
    def _(j):
        src = pl.ds(pl.multiple_of(tp * half + j * wide, wide), wide)
        at = pl.ds(pl.multiple_of(j * wide, wide), wide)
        own[:, at] = branch(src)

    swap.wait()
    summed[...] = (own[...] + other_in[...].astype(F32)).astype(BF16).reshape(n, seqs, half)
    scatter_start(n, me, tp, summed, landed, *sems(3))
    landed[me] = summed[me]
    scatter_wait(n, me, tp, summed, landed, *sems(3))
    total = lax.fori_loop(
        0, n, lambda j, acc: acc + landed[j].astype(F32), jnp.zeros((seqs, half), F32)
    )
    mine = mixed_row[:, pl.ds(pl.multiple_of(tp * half, half), half)]
    final[...] = (mine + total).astype(BF16)
    swap = pair(final, final_in, 2)
    swap.start()
    out_ref[:, pl.ds(pl.multiple_of(tp * half, half), half)] = final[...]
    swap.wait()
    out_ref[:, pl.ds(pl.multiple_of(mate * half, half), half)] = final_in[...]


def mix(n, x, retained, w_out, gain, share, open_w, weights):
    seqs, width = x.shape
    block, half, tokens = width // n, width // 2, n * seqs
    eg, eu, ed, dg, du, dd = weights
    vmem = pl.BlockSpec(memory_space=pltpu.VMEM)
    hbm = pl.BlockSpec(memory_space=pl.ANY)
    return pl.pallas_call(
        functools.partial(mix_kernel, n),
        out_shape=jax.ShapeDtypeStruct((seqs, width), BF16),
        in_specs=[vmem] * 6 + [hbm] * 6,
        out_specs=vmem,
        scratch_shapes=[
            pltpu.VMEM((n,) + retained.shape, BF16),
            pltpu.VMEM((n, seqs, block), BF16),
            pltpu.VMEM((n, seqs, block), BF16),
            pltpu.VMEM((n, seqs, block), BF16),
            pltpu.VMEM((n, seqs, block), BF16),
            pltpu.VMEM((seqs, width), F32),
            pltpu.VMEM((2, seqs, half), BF16),
            pltpu.VMEM((2, n, seqs, half), BF16),
            pltpu.VMEM(eg.shape[1:], BF16),
            pltpu.VMEM(eu.shape[1:], BF16),
            pltpu.VMEM(ed.shape[1:], BF16),
            pltpu.VMEM(dg.shape, BF16),
            pltpu.VMEM(du.shape, BF16),
            pltpu.VMEM(dd.shape, BF16),
            pltpu.VMEM((tokens, eg.shape[2]), BF16),
            pltpu.VMEM((tokens, dg.shape[1]), BF16),
            pltpu.VMEM((tokens, LANES), F32),
            pltpu.VMEM((tokens, half), BF16),
            pltpu.VMEM((tokens, half), BF16),
            pltpu.VMEM((tokens, half), F32),
            pltpu.VMEM((n, seqs, half), BF16),
            pltpu.VMEM((n, seqs, half), BF16),
            pltpu.VMEM((seqs, half), BF16),
            pltpu.VMEM((seqs, half), BF16),
            pltpu.SemaphoreType.DMA((6,)),
            pltpu.SemaphoreType.DMA((4, n)),
            pltpu.SemaphoreType.DMA((4, n)),
            pltpu.SemaphoreType.DMA((3,)),
            pltpu.SemaphoreType.DMA((3,)),
            pltpu.SemaphoreType.DMA((n,)),
            pltpu.SemaphoreType.DMA((n,)),
        ],
        compiler_params=pltpu.CompilerParams(
            collective_id=1, has_side_effects=True, vmem_limit_bytes=VMEM_LIMIT
        ),
    )(x, retained, w_out, gain, share, open_w, *weights)


def on_device(
    inputs,
    positions,
    ret_state,
    norm_mix,
    w_query,
    w_key,
    w_value,
    w_gate_in,
    head_gain,
    w_out,
    norm_ffn,
    route_ids,
    route_weight,
    exp_gate,
    exp_up,
    exp_down,
    dense_gate,
    dense_up,
    dense_down,
    branch_gate,
):
    n = lax.axis_size("ep")
    seqs, width = inputs.shape
    local_heads, head_dim = ret_state.shape[1], ret_state.shape[2]
    assert exp_gate.shape[0] == 1

    angles = rotary_angles(positions, head_dim)
    cos, sin = jnp.cos(angles), jnp.sin(angles)
    cos = jnp.concatenate([cos, cos], axis=1)
    sin = jnp.concatenate([-sin, sin], axis=1)
    gamma = jnp.exp(
        lax.dynamic_slice_in_dim(
            log_decay(HEADS), lax.axis_index("tp") * local_heads, local_heads
        )
    )
    open_w = jnp.broadcast_to(branch_gate[:, None], (width, LANES))

    joined, shares = project(
        n, inputs, norm_mix[None, :], route_ids, route_weight,
        (w_query, w_key, w_value, w_gate_in),
    )
    new_state, retained = retain(gamma, joined, head_gain[None, :], cos, sin, ret_state)
    layer_out = mix(
        n, inputs, retained, w_out, norm_ffn[None, :], shares, open_w,
        (exp_gate, exp_up, exp_down, dense_gate, dense_up, dense_down),
    )
    return (layer_out, new_state)


def solution(mesh):
    in_specs = (
        P("ep", None),
        P("ep"),
        P("ep", "tp", None, None),
        P(),
        P("ep", "tp"),
        P("ep", "tp"),
        P("ep", "tp"),
        P("ep", "tp"),
        P("tp"),
        P("tp", "ep"),
        P(),
        P("ep", None),
        P("ep", None),
        P("ep", None, "tp"),
        P("ep", None, "tp"),
        P("ep", "tp", None),
        P(None, ("ep", "tp")),
        P(None, ("ep", "tp")),
        P(("ep", "tp"), None),
        P(),
    )
    out_specs = (P("ep", None), P("ep", "tp", None, None))
    return jax.shard_map(
        on_device, mesh=mesh, in_specs=in_specs, out_specs=out_specs, check_vma=False
    )
```
